32 devices in a mesh: sp: 8 (over z, y), tp: 4 (over x, core).
Axes of the slice: x: 2, y: 2, z: 4, core: 2. Of those that a mesh axis runs over, the one named last changes fastest.
Arguments:
- residual: bfloat16 [4096, 2048], P(('sp', 'tp')), may hold values from -6 to 6
- query_proj: bfloat16 [4096, 2048], P('sp', 'tp'), may hold values from -12 to 12
- key_proj: bfloat16 [4096, 512], P('sp', 'tp'), may hold values from -12 to 12
- value_proj: bfloat16 [4096, 512], P('sp', 'tp'), may hold values from -6 to 6
- query_gain: float32 [128], replicated, may hold values from 0.4 to 4.5
- key_gain: float32 [128], replicated, may hold values from 0.4 to 4.5
- document_ids: int32 [4096], P('sp'), may hold values from 0 to 3, never falling along the last dimension, each value on 1 to 1537 neighbouring positions
- output_weight: bfloat16 [2048, 2048], replicated, may hold values from -0.125 to 0.125
- norm_gain: float32 [2048], replicated, may hold values from 0.1 to 1.9
- expert_ids: int32 [4096, 2], P(('sp', 'tp')), may hold values from 0 to 31, all different within a row; in each aligned block of 128 rows (0 to 127, 128 to 255, ...) at most 16 rows name the same one
- route_weights: float32 [4096, 2], P(('sp', 'tp')), may hold values from 0.2 to 1
- gate_weight: bfloat16 [32, 2048, 512], P(('sp', 'tp')), may hold values from -0.125 to 0.125
- up_weight: bfloat16 [32, 2048, 512], P(('sp', 'tp')), may hold values from -0.125 to 0.125
- down_weight: bfloat16 [32, 512, 2048], P(('sp', 'tp')), may hold values from -0.25 to 0.25
Outputs:
- updated: bfloat16 [4096, 2048], P(('sp', 'tp'))
The draws below stay inside these ranges and needn't reach their ends.
Inputs may be any that keep to these rules, and one draw needn't show every extreme that they name: `document_ids`: document numbers never fall along the positions; each document has at most 1537 positions, and one has exactly 1537. `expert_ids`: each row names 2 different experts; within the rows of one device no expert is named more than 16 times, and in some device's rows an expert is named exactly 16 times.
All inputs are finite; a program needn't handle non-finite values.
Results may differ from the reference program's by a relative error of at most 0.017.
Values may be sent and summed in bfloat16 or wider, within the bound.
A program may use at most 128 MiB of HBM per device.

```python
import math
import jax
import jax.numpy as jnp
import numpy as np
from jax import lax

D = 2048
HEADS = 16
KV_HEADS = 4
HEAD = 128
GRID_W = 64
FFE = 512
TOPK = 2
REACH = 3
TOK_DEV = 512
TOKENS = 4096
EROWS = 128
EXPERTS = 32
CAP = 16
DOC_MOST = 1537
DOCS = 4
N_SP = 8
N_TP = 4


def drawn(key):
    base = jax.random.fold_in(key, 7)
    key_q, key_k, key_g = jax.random.split(base, 3)
    queries = jnp.clip(jax.random.normal(key_q, (TOKENS, HEADS * HEAD), jnp.float32), -6.0, 6.0)
    keys = jnp.clip(jax.random.normal(key_k, (TOKENS, KV_HEADS * HEAD), jnp.float32), -6.0, 6.0)
    gains = jnp.exp(jax.random.uniform(key_g, (2, HEAD), jnp.float32, -0.7, 0.7))
    return (queries, keys, gains)


def draw_query_proj(key, part):
    return drawn(key)[0].astype(jnp.bfloat16)


def draw_key_proj(key, part):
    return drawn(key)[1].astype(jnp.bfloat16)


def draw_query_gain(key, part):
    return drawn(key)[2][0]


def draw_key_gain(key, part):
    return drawn(key)[2][1]


def levels(key, shape, shards, low, high):
    gain = 1.0
    for dim, parts in shards:
        heights = jax.random.uniform(jax.random.fold_in(jax.random.fold_in(key, 6), dim), (parts,), jnp.float32, low / len(shards), high / len(shards))
        gain = gain * jnp.repeat(jnp.exp(heights), shape[dim] // parts).reshape((-1,) + (1,) * (len(shape) - 1 - dim))
    return gain


def length_profile(number_of, total, most, skew):
    weights = [(1 << 20) // math.isqrt(grade ** skew) + 1 for grade in range(2, number_of + 1)]
    spare, given = total - most - (number_of - 1), [1] * (number_of - 1)
    while spare > 0:
        movable = [i for i in range(number_of - 1) if given[i] < most]
        mass, budget = sum([weights[i] for i in movable]), spare
        for i in movable:
            extra = min(most - given[i], max(1, budget * weights[i] // mass), spare)
            given[i] = given[i] + extra
            spare = spare - extra
    return np.array([most] + given)


def uneven(own_key, number_of, total, bound, skew):
    if number_of == 2:
        one = jax.random.randint(own_key, (), max(1, total - bound), min(bound, total - 1) + 1)
        return jnp.stack([one, total - one])
    lengths = jnp.asarray(length_profile(number_of, total, bound, skew), jnp.int32)
    twos = (number_of - 1) // 2
    donor, receiver = lengths[1:1 + 2 * twos:2], lengths[2:2 + 2 * twos:2]
    slack = jnp.minimum(donor - 1, bound - receiver)
    shifted = jax.random.randint(jax.random.fold_in(own_key, 1), (twos,), 0, 1 << 20) % (slack + 1)
    lengths = lengths.at[1:1 + 2 * twos:2].set(donor - shifted).at[2:2 + 2 * twos:2].set(receiver + shifted)
    return lengths[jax.random.permutation(jax.random.fold_in(own_key, 2), number_of)]


def assign_block(stream_key, own, number, rows, number_of, top, reach, lean):
    order = jax.random.permutation(stream_key, number_of)
    packed, common = shares(number_of, rows * top, reach, lean, True), shares(number_of, rows * top, reach, lean, False)
    places = jnp.arange(number_of)

    def named(tallies, offset_by):
        used = int((tallies > 0).sum())
        fixed = max(1, used // 4)
        shifted = fixed + (places - fixed + offset_by * (used - fixed)) % max(1, number_of - fixed)
        return jnp.zeros((number_of,), jnp.int32).at[order[jnp.where(places < fixed, places, shifted)]].set(jnp.asarray(tallies, jnp.int32))

    tallies = jnp.where(number % 4 == 0, named(packed, number // 4), named(common, number - number // 4 - 1))
    mixed = jax.random.permutation(jax.random.fold_in(own, 3), number_of)
    source_of, taker = mixed[0:number_of // 2 * 2:2], mixed[1:number_of // 2 * 2:2]
    room = jnp.minimum(tallies[source_of] - 1, reach - tallies[taker]) // 2
    room = jnp.where((source_of == order[0]) | (taker == order[0]) | (tallies[taker] == 0), 0, jnp.maximum(room, 0))
    shifted = jax.random.randint(jax.random.fold_in(own, 4), (number_of // 2,), 0, 1 << 20) % (room + 1)
    tallies = tallies.at[source_of].add(-shifted).at[taker].add(shifted)
    members = jnp.searchsorted(jnp.cumsum(tallies), jnp.arange(rows * top), side="right").astype(jnp.int32)
    table = members.reshape(top, rows).T
    table = table[jax.random.permutation(jax.random.fold_in(own, 1), rows)]
    offset_by = jax.random.randint(jax.random.fold_in(own, 2), (rows, 1), 0, top)
    return jnp.take_along_axis(table, (jnp.arange(top)[None, :] + offset_by) % top, axis=1)


def shares(number_of, total, most, lean, full):
    portions = [(1 << 20) // math.isqrt(standing ** lean) + 1 for standing in range(1, number_of + 1)]
    largest = most if full else min(most, max(-(-total // number_of), total * portions[0] // sum(portions)))
    least = 1 if total - largest >= number_of - 1 else 0
    given, surplus = [largest] + [least] * (number_of - 1), total - largest - least * (number_of - 1)
    while surplus > 0:
        candidates = [i for i in range(1, number_of) if given[i] < largest] or [i for i in range(1, number_of) if given[i] < most]
        whole, remaining = sum([portions[i] for i in candidates]), surplus
        for i in candidates:
            extra = min(most - given[i], max(1, remaining * portions[i] // whole), surplus)
            given[i] = given[i] + extra
            surplus = surplus - extra
    return np.array(given)


def centred(own_key, extent, width, bound, pieces=(), kind=jnp.bfloat16):
    factor_of = levels(own_key, extent, pieces, -0.22, 0.18) if pieces else 1.0
    values = jax.random.normal(own_key, extent, jnp.float32) * width * factor_of
    return jnp.minimum(jnp.maximum(values, -bound), bound).astype(kind)


def setup_inputs(seed: int = 0) -> dict:
    arg_keys = jax.random.split(jax.random.key(seed), 15)
    residual = centred(arg_keys[0], (TOKENS, D), 1.0, 6.0, ((0, 32),))
    query_proj = draw_query_proj(jax.random.fold_in(arg_keys[14], 71), 0)
    key_proj = draw_key_proj(jax.random.fold_in(arg_keys[14], 71), 0)
    value_proj = centred(arg_keys[3], (TOKENS, KV_HEADS * HEAD), 1.0, 6.0, ((0, 8), (1, 4)))
    query_gain = draw_query_gain(jax.random.fold_in(arg_keys[14], 71), 0)
    key_gain = draw_key_gain(jax.random.fold_in(arg_keys[14], 71), 0)
    document_ids = jnp.searchsorted(jnp.cumsum(uneven(arg_keys[6], DOCS, TOKENS, DOC_MOST, 2)), jnp.arange(TOKENS), side="right").astype(jnp.int32)
    output_weight = centred(arg_keys[7], (HEADS * HEAD, D), (HEADS * HEAD) ** -0.5, 0.125)
    norm_gain = jnp.clip(1.0 + 0.18 * jax.random.normal(arg_keys[8], (D,), jnp.float32), 0.1, 1.9)
    expert_ids_keys = jax.random.split(jax.random.fold_in(arg_keys[9], 1), TOKENS // EROWS)
    expert_ids_turns = jax.random.permutation(jax.random.fold_in(arg_keys[9], 3), TOKENS // EROWS)
    expert_ids = jax.vmap(lambda own, number: assign_block(jax.random.fold_in(arg_keys[9], 2), own, number, EROWS, EXPERTS, TOPK, CAP, 2))(expert_ids_keys, expert_ids_turns).reshape((TOKENS, TOPK))
    route_weights = jnp.clip(0.2 + 0.8 * jax.random.uniform(arg_keys[10], (TOKENS, TOPK), jnp.float32) ** levels(arg_keys[10], (TOKENS, TOPK), ((0, 32),), -0.2, 0.2), 0.2, 1.0)
    gate_weight = centred(arg_keys[11], (EXPERTS, D, FFE), D ** -0.5, 0.125, ((0, 32),))
    up_weight = centred(arg_keys[12], (EXPERTS, D, FFE), D ** -0.5, 0.125, ((0, 32),))
    down_weight = centred(arg_keys[13], (EXPERTS, FFE, D), FFE ** -0.5, 0.25, ((0, 32),))
    return dict(residual=residual, query_proj=query_proj, key_proj=key_proj, value_proj=value_proj, query_gain=query_gain, key_gain=key_gain, document_ids=document_ids, output_weight=output_weight, norm_gain=norm_gain, expert_ids=expert_ids, route_weights=route_weights, gate_weight=gate_weight, up_weight=up_weight, down_weight=down_weight)


norm_eps = 1e-06
rope_base = 10000.0

def rotary_tables(first_row, length):
    freq_count = HEAD // 4
    inverse = 1.0 / rope_base ** (jnp.arange(freq_count, dtype=jnp.float32) / freq_count)
    position = first_row + jnp.arange(length, dtype=jnp.int32)
    grid_row = (position // GRID_W).astype(jnp.float32)
    grid_col = (position % GRID_W).astype(jnp.float32)
    angles = jnp.concatenate([grid_row[:, None] * inverse[None, :], grid_col[:, None] * inverse[None, :]], axis=1)
    return (jnp.cos(angles), jnp.sin(angles))

def norm_rotate(projected, gains, cosine, sine_table):
    length = projected.shape[0]
    values_wide = projected.astype(jnp.float32).reshape(length, -1, HEAD)
    scaled = values_wide * lax.rsqrt(lax.optimization_barrier(jnp.mean(values_wide * values_wide, axis=-1, keepdims=True)) + norm_eps) * gains
    half_size = HEAD // 2
    first_half = scaled[..., :half_size]
    second_half = scaled[..., half_size:]
    cosine_rows = cosine[:, None, :]
    sine_rows = sine_table[:, None, :]
    turned = jnp.concatenate([first_half * cosine_rows - second_half * sine_rows, first_half * sine_rows + second_half * cosine_rows], axis=-1)
    return turned.reshape(length, -1).astype(jnp.bfloat16)

def attend(query_block, key_block, value_block, query_doc, key_doc, groups):
    query_rows = query_block.shape[0]
    key_rows = key_block.shape[0]
    key_heads = key_block.shape[1] // HEAD
    query_grid = query_block.astype(jnp.float32).reshape(query_rows, key_heads, groups, HEAD)
    key_grid = key_block.astype(jnp.float32).reshape(key_rows, key_heads, HEAD)
    value_grid = value_block.astype(jnp.float32).reshape(key_rows, key_heads, HEAD)
    scores = jnp.einsum('qhgd,khd->hgqk', query_grid, key_grid) * HEAD ** (-0.5)
    same_doc = query_doc[:, None] == key_doc[None, :]
    scores = jnp.where(same_doc[None, None], scores, -jnp.inf)
    row_max = lax.optimization_barrier(jnp.max(scores, axis=-1, keepdims=True))
    weights = jnp.exp(scores - row_max)
    denominator = lax.optimization_barrier(jnp.sum(weights, axis=-1))
    rounded = weights.astype(jnp.bfloat16).astype(jnp.float32)
    weighted = jnp.einsum('hgqk,khd->hgqd', rounded, value_grid) / denominator[..., None]
    return jnp.transpose(weighted, (2, 0, 1, 3)).reshape(query_rows, key_heads * groups * HEAD).astype(jnp.bfloat16)

def reference(residual, query_proj, key_proj, value_proj, query_gain, key_gain, document_ids, output_weight, norm_gain, expert_ids, route_weights, gate_weight, up_weight, down_weight):
    tokens = query_proj.shape[0]
    cosine, sine_table = rotary_tables(jnp.int32(0), tokens)
    query_norm = norm_rotate(query_proj, query_gain, cosine, sine_table)
    key_norm = norm_rotate(key_proj, key_gain, cosine, sine_table)
    groups = HEADS // KV_HEADS
    window = min(tokens, TOK_DEV + 2 * REACH * TOK_DEV)

    def one_block(block_index):
        first_row = block_index * TOK_DEV
        key_first = jnp.clip(first_row - REACH * TOK_DEV, 0, tokens - window).astype(jnp.int32)
        query_block = lax.dynamic_slice_in_dim(query_norm, first_row, TOK_DEV, 0)
        query_doc = lax.dynamic_slice_in_dim(document_ids, first_row, TOK_DEV, 0)
        key_block = lax.dynamic_slice_in_dim(key_norm, key_first, window, 0)
        value_block = lax.dynamic_slice_in_dim(value_proj, key_first, window, 0)
        key_doc = lax.dynamic_slice_in_dim(document_ids, key_first, window, 0)
        return attend(query_block, key_block, value_block, query_doc, key_doc, groups)
    attn = lax.map(one_block, jnp.arange(tokens // TOK_DEV, dtype=jnp.int32)).reshape(tokens, HEADS * HEAD)
    hidden = (residual.astype(jnp.float32) + jnp.dot(attn, output_weight, preferred_element_type=jnp.float32)).astype(jnp.bfloat16)
    hidden_wide = hidden.astype(jnp.float32)
    normed = (hidden_wide * lax.rsqrt(lax.optimization_barrier(jnp.mean(hidden_wide * hidden_wide, axis=-1, keepdims=True)) + norm_eps) * norm_gain).astype(jnp.bfloat16)
    flat_ids = expert_ids.reshape(-1)
    flat_weights = route_weights.reshape(-1)
    top_count = expert_ids.shape[1]
    limit = N_SP * N_TP * CAP
    slot_numbers = jnp.arange(limit, dtype=jnp.int32)

    def add_expert(expert_index, running):
        matches = flat_ids == expert_index
        count = jnp.sum(matches.astype(jnp.int32))
        picked = jnp.nonzero(matches, size=limit, fill_value=0)[0].astype(jnp.int32)
        valid = (slot_numbers < count).astype(jnp.float32)
        token_index = picked // top_count
        chosen = normed[token_index]
        gate_part = jnp.dot(chosen, gate_weight[expert_index], preferred_element_type=jnp.float32)
        up_part = jnp.dot(chosen, up_weight[expert_index], preferred_element_type=jnp.float32)
        activity = (jax.nn.silu(gate_part) * up_part).astype(jnp.bfloat16)
        expert_out = jnp.dot(activity, down_weight[expert_index], preferred_element_type=jnp.float32).astype(jnp.bfloat16)
        factor = (flat_weights[picked] * valid)[:, None]
        return running.at[token_index].add(factor * expert_out.astype(jnp.float32))
    combined = lax.fori_loop(0, EXPERTS, add_expert, jnp.zeros((tokens, D), jnp.float32))
    return (hidden_wide + combined).astype(jnp.bfloat16)
```

```python
import functools
import math

import jax
import jax.numpy as jnp
from jax import lax
from jax.experimental import pallas as pl
from jax.experimental.pallas import tpu as pltpu
from jax.sharding import PartitionSpec as P

HEAD = 128
GRID_W = 64
REACH = 3


norm_eps = 1e-06
rope_base = 10000.0
masked_low = -1e30
MESH = pl.DeviceIdType.MESH
DOC_KEY = 128.0
DOC_QUERY = 64.0
EXP2_SCALE = math.log2(math.e) / math.sqrt(HEAD)


def rotary_tables(first_row, length):
    freq_count = HEAD // 4
    inverse = 1.0 / rope_base ** (jnp.arange(freq_count, dtype=jnp.float32) / freq_count)
    position = first_row + jnp.arange(length, dtype=jnp.int32)
    grid_row = (position // GRID_W).astype(jnp.float32)
    grid_col = (position % GRID_W).astype(jnp.float32)
    angles = jnp.concatenate(
        [grid_row[:, None] * inverse[None, :], grid_col[:, None] * inverse[None, :]], axis=1
    )
    return (jnp.cos(angles), jnp.sin(angles))


def norm_rotate(projected, gains, cosine, sine_table):
    length = projected.shape[0]
    values_wide = projected.astype(jnp.float32).reshape(length, -1, HEAD)
    scaled = (
        values_wide
        * lax.rsqrt(jnp.mean(values_wide * values_wide, axis=-1, keepdims=True) + norm_eps)
        * gains
    )
    half_size = HEAD // 2
    first_half = scaled[..., :half_size]
    second_half = scaled[..., half_size:]
    cosine_rows = cosine[:, None, :]
    sine_rows = sine_table[:, None, :]
    turned = jnp.concatenate(
        [
            first_half * cosine_rows - second_half * sine_rows,
            first_half * sine_rows + second_half * cosine_rows,
        ],
        axis=-1,
    )
    return turned.reshape(length, -1).astype(jnp.bfloat16)


def attention_kernel(
    n_sp, n_tp, q_ref, k_ref, vt_ref, doc_ref, res_ref, gain_ref, wo_hbm,
    hid_ref, nrm_ref,
    wo_v, k_in, vt_in, doc_in, k_aug, m_s, l_s, acc_s, att_s, all_s,
    send, recv, t_send, t_recv, w_sem,
):
    sp = lax.axis_index("sp")
    tp = lax.axis_index("tp")
    heads = q_ref.shape[0]
    rows = res_ref.shape[0]
    width = att_s.shape[1]
    slots = 2 * REACH

    def distance(j):
        return (j // 2 + 1) * (1 - 2 * (j % 2))

    def inside(index):
        return jnp.logical_and(index >= 0, index < n_sp)

    wo_copy = pltpu.make_async_copy(wo_hbm, wo_v, w_sem)
    wo_copy.start()

    barrier = pltpu.get_barrier_semaphore()
    for j in range(slots):
        there = sp + distance(j)

        @pl.when(inside(there))
        def _():
            pl.semaphore_signal(barrier, inc=1, device_id=(there, tp), device_id_type=MESH)

    for k in range(1, n_tp):
        pl.semaphore_signal(
            barrier, inc=1, device_id=(sp, lax.rem(tp + k, n_tp)), device_id_type=MESH
        )
    beside = jnp.minimum(sp, REACH) + jnp.minimum(n_sp - 1 - sp, REACH)
    pl.semaphore_wait(barrier, n_tp - 1 + beside)

    def copies(j):
        there = (sp + distance(j), tp)
        return [
            pltpu.make_async_remote_copy(
                src_ref=one,
                dst_ref=into.at[j],
                send_sem=send.at[j, i],
                recv_sem=recv.at[j, i],
                device_id=there,
                device_id_type=MESH,
            )
            for i, (one, into) in enumerate(((k_ref, k_in), (vt_ref, vt_in), (doc_ref, doc_in)))
        ]

    for j in range(slots):

        @pl.when(inside(sp + distance(j)))
        def _():
            for copy in copies(j):
                copy.start()

    def take(keys, values_t, docs, first):
        length = keys.shape[0]
        doc_col = jnp.broadcast_to(docs[0:1, :], (HEAD, length)).T
        lanes = lax.broadcasted_iota(jnp.int32, (length, HEAD), 1).astype(jnp.float32)
        k_aug[:, :HEAD] = keys[...]
        k_aug[:, HEAD:] = jnp.where(doc_col == lanes, DOC_KEY, 0.0).astype(jnp.bfloat16)
        for h in range(heads):
            s = jnp.dot(k_aug[...], q_ref[h], preferred_element_type=jnp.float32)
            top = jnp.max(s, axis=0, keepdims=True)
            if not first:
                top = jnp.maximum(m_s[h], top)
            e = jnp.exp2((s - top) * EXP2_SCALE)
            den = jnp.sum(e, axis=0, keepdims=True)
            part = jnp.dot(
                values_t[...], e.astype(jnp.bfloat16), preferred_element_type=jnp.float32
            )
            if first:
                l_s[h] = den
                acc_s[h] = part
            else:
                old = jnp.exp2((m_s[h] - top) * EXP2_SCALE)
                l_s[h] = l_s[h] * old + den
                acc_s[h] = acc_s[h] * old + part
            m_s[h] = top

    take(k_ref, vt_ref, doc_ref, True)

    def step(j, carry):
        @pl.when(inside(sp - distance(j)))
        def _():
            for copy in copies(j):
                copy.wait_recv()
            take(k_in.at[j], vt_in.at[j], doc_in.at[j], False)

        return carry

    lax.fori_loop(0, slots, step, 0)

    for h in range(heads):
        out = acc_s[h] / l_s[h]
        att_s[:, h * HEAD : (h + 1) * HEAD] = out.T.astype(jnp.bfloat16)

    def exchange(k):
        there = lax.rem(tp + k, n_tp)
        return pltpu.make_async_remote_copy(
            src_ref=att_s.at[pl.ds(pl.multiple_of(there * rows, rows), rows), :],
            dst_ref=all_s.at[tp],
            send_sem=t_send.at[k],
            recv_sem=t_recv.at[k],
            device_id=(sp, there),
            device_id_type=MESH,
        )

    for k in range(n_tp - 1, 0, -1):
        exchange(k).start()
    wo_copy.wait()

    def weight_rows(i):
        return wo_v[pl.ds(pl.multiple_of(i * width, width), width), :]

    projected = jnp.dot(
        att_s[pl.ds(pl.multiple_of(tp * rows, rows), rows), :],
        weight_rows(tp),
        preferred_element_type=jnp.float32,
    )
    for k in range(1, n_tp):
        exchange(k).wait_recv()
        source = lax.rem(tp - k + n_tp, n_tp)
        projected += jnp.dot(
            all_s[source], weight_rows(source), preferred_element_type=jnp.float32
        )
    hidden = (res_ref[...].astype(jnp.float32) + projected).astype(jnp.bfloat16)
    hid_ref[...] = hidden
    wide = hidden.astype(jnp.float32)
    mean = jnp.mean(wide * wide, axis=-1, keepdims=True)
    nrm_ref[...] = (wide * lax.rsqrt(mean + norm_eps) * gain_ref[...]).astype(jnp.bfloat16)

    for j in range(slots):

        @pl.when(inside(sp + distance(j)))
        def _():
            for copy in copies(j):
                copy.wait_send()

    for k in range(1, n_tp):
        exchange(k).wait_send()


def attend(q_aug, key_norm, value_t, doc_rows, residual, norm_gain, output_weight):
    n_sp, n_tp = lax.axis_size("sp"), lax.axis_size("tp")
    heads, deep, length = q_aug.shape
    rows, model = residual.shape
    vmem = pl.BlockSpec(memory_space=pltpu.VMEM)
    slots = 2 * REACH
    return pl.pallas_call(
        functools.partial(attention_kernel, n_sp, n_tp),
        out_shape=[jax.ShapeDtypeStruct((rows, model), jnp.bfloat16)] * 2,
        in_specs=[vmem] * 6 + [pl.BlockSpec(memory_space=pl.ANY)],
        out_specs=[vmem] * 2,
        scratch_shapes=[
            pltpu.VMEM(output_weight.shape, jnp.bfloat16),
            pltpu.VMEM((slots,) + key_norm.shape, jnp.bfloat16),
            pltpu.VMEM((slots,) + value_t.shape, jnp.bfloat16),
            pltpu.VMEM((slots,) + doc_rows.shape, jnp.float32),
            pltpu.VMEM((length, deep), jnp.bfloat16),
            pltpu.VMEM((heads, 1, length), jnp.float32),
            pltpu.VMEM((heads, 1, length), jnp.float32),
            pltpu.VMEM((heads, HEAD, length), jnp.float32),
            pltpu.VMEM((length, heads * HEAD), jnp.bfloat16),
            pltpu.VMEM((n_tp, rows, heads * HEAD), jnp.bfloat16),
            pltpu.SemaphoreType.DMA((slots, 3)),
            pltpu.SemaphoreType.DMA((slots, 3)),
            pltpu.SemaphoreType.DMA((n_tp,)),
            pltpu.SemaphoreType.DMA((n_tp,)),
            pltpu.SemaphoreType.DMA(()),
        ],
        compiler_params=pltpu.CompilerParams(
            collective_id=1, has_side_effects=True, vmem_limit_bytes=48 * 1024 * 1024
        ),
    )(q_aug, key_norm, value_t, doc_rows, residual, norm_gain.reshape(1, -1), output_weight)


def on_device(
    residual,
    query_proj,
    key_proj,
    value_proj,
    query_gain,
    key_gain,
    document_ids,
    output_weight,
    norm_gain,
    expert_ids,
    route_weights,
    gate_weight,
    up_weight,
    down_weight,
):
    rows_here = query_proj.shape[0]
    cosine, sine_table = rotary_tables(lax.axis_index("sp") * rows_here, rows_here)
    query_norm = norm_rotate(query_proj, query_gain, cosine, sine_table)
    key_norm = norm_rotate(key_proj, key_gain, cosine, sine_table)
    heads = query_proj.shape[1] // HEAD
    docs = document_ids.astype(jnp.float32)
    query_t = jnp.transpose(query_norm.reshape(rows_here, heads, HEAD), (1, 2, 0))
    query_doc = jnp.where(
        docs[None, :] == jnp.arange(HEAD, dtype=jnp.float32)[:, None], DOC_QUERY, 0.0
    ).astype(jnp.bfloat16)
    q_aug = jnp.concatenate(
        [query_t, jnp.broadcast_to(query_doc[None], (heads, HEAD, rows_here))], axis=1
    )
    doc_rows = jnp.broadcast_to(docs[None, :], (8, rows_here))
    hidden, normed = attend(
        q_aug, key_norm, value_proj.T, doc_rows, residual, norm_gain, output_weight
    )
    token_rows = residual.shape[0]
    top_count = expert_ids.shape[1]
    experts_all = lax.axis_size("sp") * lax.axis_size("tp")
    capacity = max(2, 2 * token_rows * top_count // experts_all)
    flat_ids = expert_ids.reshape(-1)
    onehot = (flat_ids[:, None] == jnp.arange(experts_all, dtype=jnp.int32)[None, :]).astype(
        jnp.int32
    )
    arrival = jnp.sum(jnp.cumsum(onehot, axis=0) * onehot, axis=1) - 1
    slot_index = flat_ids * capacity + arrival
    slot_grid = slot_index.reshape(token_rows, top_count)
    placing = jnp.sum(
        (
            jnp.arange(experts_all * capacity, dtype=jnp.int32)[:, None, None] == slot_grid[None]
        ).astype(jnp.float32),
        axis=2,
    ).astype(jnp.bfloat16)
    outgoing = jnp.dot(placing, normed, preferred_element_type=jnp.float32).astype(jnp.bfloat16)
    outgoing = outgoing.reshape(experts_all, capacity, normed.shape[1])
    arrived = lax.all_to_all(outgoing, ("sp", "tp"), split_axis=0, concat_axis=0, tiled=True)
    sources, slots, width = arrived.shape
    flat_rows = arrived.reshape(sources * slots, width)
    gate_part = jnp.dot(flat_rows, gate_weight[0], preferred_element_type=jnp.float32)
    up_part = jnp.dot(flat_rows, up_weight[0], preferred_element_type=jnp.float32)
    activity = (jax.nn.silu(gate_part) * up_part).astype(jnp.bfloat16)
    expert_out = jnp.dot(activity, down_weight[0], preferred_element_type=jnp.float32).astype(
        jnp.bfloat16
    )
    returned = lax.all_to_all(
        expert_out.reshape(sources, slots, width),
        ("sp", "tp"),
        split_axis=0,
        concat_axis=0,
        tiled=True,
    )
    spread = jnp.sum(
        jnp.where(
            jnp.arange(experts_all * capacity, dtype=jnp.int32)[None, None, :]
            == slot_grid[:, :, None],
            route_weights[:, :, None],
            0.0,
        ),
        axis=1,
    )
    high = spread.astype(jnp.bfloat16)
    low = (spread - high.astype(jnp.float32)).astype(jnp.bfloat16)
    rows_back = returned.reshape(experts_all * capacity, -1)
    combined = jnp.dot(high, rows_back, preferred_element_type=jnp.float32) + jnp.dot(
        low, rows_back, preferred_element_type=jnp.float32
    )
    return (hidden.astype(jnp.float32) + combined).astype(jnp.bfloat16)


def solution(mesh):
    in_specs = (
        P(("sp", "tp"), None),
        P("sp", "tp"),
        P("sp", "tp"),
        P("sp", "tp"),
        P(),
        P(),
        P("sp"),
        P(),
        P(),
        P(("sp", "tp"), None),
        P(("sp", "tp"), None),
        P(("sp", "tp"), None, None),
        P(("sp", "tp"), None, None),
        P(("sp", "tp"), None, None),
    )
    out_specs = P(("sp", "tp"), None)
    return jax.shard_map(
        on_device, mesh=mesh, in_specs=in_specs, out_specs=out_specs, check_vma=False
    )
```

```python
import functools
import math

import jax
import jax.numpy as jnp
from jax import lax
from jax.experimental import pallas as pl
from jax.experimental.pallas import tpu as pltpu
from jax.sharding import PartitionSpec as P

HEAD = 128
GRID_W = 64
REACH = 3


norm_eps = 1e-06
rope_base = 10000.0
masked_low = -1e30
MESH = pl.DeviceIdType.MESH
DOC_KEY = 128.0
DOC_QUERY = 64.0
EXP2_SCALE = math.log2(math.e) / math.sqrt(HEAD)


def rotary_tables(first_row, length):
    freq_count = HEAD // 4
    inverse = 1.0 / rope_base ** (jnp.arange(freq_count, dtype=jnp.float32) / freq_count)
    position = first_row + jnp.arange(length, dtype=jnp.int32)
    grid_row = (position // GRID_W).astype(jnp.float32)
    grid_col = (position % GRID_W).astype(jnp.float32)
    angles = jnp.concatenate(
        [grid_row[:, None] * inverse[None, :], grid_col[:, None] * inverse[None, :]], axis=1
    )
    return (jnp.cos(angles), jnp.sin(angles))


def norm_rotate(projected, gains, cosine, sine_table):
    length = projected.shape[0]
    values_wide = projected.astype(jnp.float32).reshape(length, -1, HEAD)
    scaled = (
        values_wide
        * lax.rsqrt(jnp.mean(values_wide * values_wide, axis=-1, keepdims=True) + norm_eps)
        * gains
    )
    half_size = HEAD // 2
    first_half = scaled[..., :half_size]
    second_half = scaled[..., half_size:]
    cosine_rows = cosine[:, None, :]
    sine_rows = sine_table[:, None, :]
    turned = jnp.concatenate(
        [
            first_half * cosine_rows - second_half * sine_rows,
            first_half * sine_rows + second_half * cosine_rows,
        ],
        axis=-1,
    )
    return turned.reshape(length, -1).astype(jnp.bfloat16)


def attention_kernel(
    n_sp, n_tp, q_ref, k_ref, vt_ref, doc_ref, res_ref, gain_ref, wo_hbm,
    hid_ref, nrm_ref,
    wo_v, k_in, vt_in, doc_in, k_aug, m_s, l_s, acc_s, att_s, all_s,
    send, recv, t_send, t_recv, w_sem,
):
    sp = lax.axis_index("sp")
    tp = lax.axis_index("tp")
    heads = q_ref.shape[0]
    rows = res_ref.shape[0]
    width = att_s.shape[1]
    slots = 2 * REACH

    def distance(j):
        return (j // 2 + 1) * (1 - 2 * (j % 2))

    def inside(index):
        return jnp.logical_and(index >= 0, index < n_sp)

    wo_copy = pltpu.make_async_copy(wo_hbm, wo_v, w_sem)
    wo_copy.start()

    barrier = pltpu.get_barrier_semaphore()
    for j in range(slots):
        there = sp + distance(j)

        @pl.when(inside(there))
        def _():
            pl.semaphore_signal(barrier, inc=1, device_id=(there, tp), device_id_type=MESH)

    for k in range(1, n_tp):
        pl.semaphore_signal(
            barrier, inc=1, device_id=(sp, lax.rem(tp + k, n_tp)), device_id_type=MESH
        )
    beside = jnp.minimum(sp, REACH) + jnp.minimum(n_sp - 1 - sp, REACH)
    pl.semaphore_wait(barrier, n_tp - 1 + beside)

    def copies(j):
        there = (sp + distance(j), tp)
        return [
            pltpu.make_async_remote_copy(
                src_ref=one,
                dst_ref=into.at[j],
                send_sem=send.at[j, i],
                recv_sem=recv.at[j, i],
                device_id=there,
                device_id_type=MESH,
            )
            for i, (one, into) in enumerate(((k_ref, k_in), (vt_ref, vt_in), (doc_ref, doc_in)))
        ]

    for j in range(slots):

        @pl.when(inside(sp + distance(j)))
        def _():
            for copy in copies(j):
                copy.start()

    def take(keys, values_t, docs, first):
        length = keys.shape[0]
        doc_col = jnp.broadcast_to(docs[0:1, :], (HEAD, length)).T
        lanes = lax.broadcasted_iota(jnp.int32, (length, HEAD), 1).astype(jnp.float32)
        k_aug[:, :HEAD] = keys[...]
        k_aug[:, HEAD:] = jnp.where(doc_col == lanes, DOC_KEY, 0.0).astype(jnp.bfloat16)
        for h in range(heads):
            s = jnp.dot(k_aug[...], q_ref[h], preferred_element_type=jnp.float32)
            top = jnp.max(s, axis=0, keepdims=True)
            if not first:
                top = jnp.maximum(m_s[h], top)
            e = jnp.exp2((s - top) * EXP2_SCALE)
            den = jnp.sum(e, axis=0, keepdims=True)
            part = jnp.dot(
                values_t[...], e.astype(jnp.bfloat16), preferred_element_type=jnp.float32
            )
            if first:
                l_s[h] = den
                acc_s[h] = part
            else:
                old = jnp.exp2((m_s[h] - top) * EXP2_SCALE)
                l_s[h] = l_s[h] * old + den
                acc_s[h] = acc_s[h] * old + part
            m_s[h] = top

    take(k_ref, vt_ref, doc_ref, True)

    def step(j, carry):
        @pl.when(inside(sp - distance(j)))
        def _():
            for copy in copies(j):
                copy.wait_recv()
            take(k_in.at[j], vt_in.at[j], doc_in.at[j], False)

        return carry

    lax.fori_loop(0, slots, step, 0)

    for h in range(heads):
        out = acc_s[h] / l_s[h]
        att_s[:, h * HEAD : (h + 1) * HEAD] = out.T.astype(jnp.bfloat16)

    def exchange(k):
        there = lax.rem(tp + k, n_tp)
        return pltpu.make_async_remote_copy(
            src_ref=att_s.at[pl.ds(pl.multiple_of(there * rows, rows), rows), :],
            dst_ref=all_s.at[tp],
            send_sem=t_send.at[k],
            recv_sem=t_recv.at[k],
            device_id=(sp, there),
            device_id_type=MESH,
        )

    for k in range(n_tp - 1, 0, -1):
        exchange(k).start()
    wo_copy.wait()

    def weight_rows(i):
        return wo_v[pl.ds(pl.multiple_of(i * width, width), width), :]

    projected = jnp.dot(
        att_s[pl.ds(pl.multiple_of(tp * rows, rows), rows), :],
        weight_rows(tp),
        preferred_element_type=jnp.float32,
    )
    for k in range(1, n_tp):
        exchange(k).wait_recv()
        source = lax.rem(tp - k + n_tp, n_tp)
        projected += jnp.dot(
            all_s[source], weight_rows(source), preferred_element_type=jnp.float32
        )
    hidden = (res_ref[...].astype(jnp.float32) + projected).astype(jnp.bfloat16)
    hid_ref[...] = hidden
    wide = hidden.astype(jnp.float32)
    mean = jnp.mean(wide * wide, axis=-1, keepdims=True)
    nrm_ref[...] = (wide * lax.rsqrt(mean + norm_eps) * gain_ref[...]).astype(jnp.bfloat16)

    for j in range(slots):

        @pl.when(inside(sp + distance(j)))
        def _():
            for copy in copies(j):
                copy.wait_send()

    for k in range(1, n_tp):
        exchange(k).wait_send()


def attend(q_aug, key_norm, value_t, doc_rows, residual, norm_gain, output_weight):
    n_sp, n_tp = lax.axis_size("sp"), lax.axis_size("tp")
    heads, deep, length = q_aug.shape
    rows, model = residual.shape
    vmem = pl.BlockSpec(memory_space=pltpu.VMEM)
    slots = 2 * REACH
    return pl.pallas_call(
        functools.partial(attention_kernel, n_sp, n_tp),
        out_shape=[jax.ShapeDtypeStruct((rows, model), jnp.bfloat16)] * 2,
        in_specs=[vmem] * 6 + [pl.BlockSpec(memory_space=pl.ANY)],
        out_specs=[vmem] * 2,
        scratch_shapes=[
            pltpu.VMEM(output_weight.shape, jnp.bfloat16),
            pltpu.VMEM((slots,) + key_norm.shape, jnp.bfloat16),
            pltpu.VMEM((slots,) + value_t.shape, jnp.bfloat16),
            pltpu.VMEM((slots,) + doc_rows.shape, jnp.float32),
            pltpu.VMEM((length, deep), jnp.bfloat16),
            pltpu.VMEM((heads, 1, length), jnp.float32),
            pltpu.VMEM((heads, 1, length), jnp.float32),
            pltpu.VMEM((heads, HEAD, length), jnp.float32),
            pltpu.VMEM((length, heads * HEAD), jnp.bfloat16),
            pltpu.VMEM((n_tp, rows, heads * HEAD), jnp.bfloat16),
            pltpu.SemaphoreType.DMA((slots, 3)),
            pltpu.SemaphoreType.DMA((slots, 3)),
            pltpu.SemaphoreType.DMA((n_tp,)),
            pltpu.SemaphoreType.DMA((n_tp,)),
            pltpu.SemaphoreType.DMA(()),
        ],
        compiler_params=pltpu.CompilerParams(
            collective_id=1, has_side_effects=True, vmem_limit_bytes=48 * 1024 * 1024
        ),
    )(q_aug, key_norm, value_t, doc_rows, residual, norm_gain.reshape(1, -1), output_weight)


def expert_kernel(
    n_tp, capacity, out_ref, high_ref, low_ref, hid_ref, gate_hbm, up_hbm, down_hbm,
    new_ref,
    gate_v, up_v, down_v, arrived, answer, returned,
    d_send, d_recv, r_send, r_recv, w_sem,
):
    me = lax.axis_index("sp") * n_tp + lax.axis_index("tp")
    devices = out_ref.shape[0] // capacity
    rows = hid_ref.shape[0]
    members = rows // capacity
    groups = devices // members
    my_group = lax.div(me, members)
    my_place = lax.rem(me, members)

    loads = [
        pltpu.make_async_copy(source.at[0], into, w_sem.at[i])
        for i, (source, into) in enumerate(
            ((gate_hbm, gate_v), (up_hbm, up_v), (down_hbm, down_v))
        )
    ]
    for load in loads:
        load.start()

    def place(device):
        return (lax.div(device, n_tp), lax.rem(device, n_tp))

    def slots(device):
        return pl.ds(pl.multiple_of(device * capacity, capacity), capacity)

    barrier = pltpu.get_barrier_semaphore()

    def greet(i, carry):
        there = lax.rem(me + i, devices)
        pl.semaphore_signal(barrier, inc=1, device_id=place(there), device_id_type=MESH)
        return carry

    lax.fori_loop(1, devices, greet, 0)
    pl.semaphore_wait(barrier, devices - 1)

    def dispatch(device, landing):
        return pltpu.make_async_remote_copy(
            src_ref=out_ref.at[slots(device)],
            dst_ref=arrived.at[slots(landing)],
            send_sem=d_send.at[device],
            recv_sem=d_recv.at[landing],
            device_id=place(device),
            device_id_type=MESH,
        )

    def give_back(device, landing):
        return pltpu.make_async_remote_copy(
            src_ref=answer.at[slots(device)],
            dst_ref=returned.at[slots(landing)],
            send_sem=r_send.at[device],
            recv_sem=r_recv.at[landing],
            device_id=place(device),
            device_id_type=MESH,
        )

    def each(group, skip_self, act):
        def one(i, carry):
            act(group * members + lax.rem(my_place + i, members))
            return carry

        lax.fori_loop(1 if skip_self else 0, members, one, 0)

    def group_at(step):
        return lax.rem(my_group + step + groups, groups)

    def group_rows(group):
        return pl.ds(pl.multiple_of(group * rows, rows), rows)

    for c in range(groups):
        each(group_at(c), c == 0, lambda device: dispatch(device, me).start())
    arrived[slots(me), :] = out_ref[slots(me), :]
    for load in loads:
        load.wait()

    for c in range(groups):
        group = group_at(-c)
        each(group, c == 0, lambda device: dispatch(device, device).wait_recv())
        x = arrived[group_rows(group), :]
        gate_part = jnp.dot(x, gate_v[...], preferred_element_type=jnp.float32)
        up_part = jnp.dot(x, up_v[...], preferred_element_type=jnp.float32)
        activity = (jax.nn.silu(gate_part) * up_part).astype(jnp.bfloat16)
        answer[group_rows(group), :] = jnp.dot(
            activity, down_v[...], preferred_element_type=jnp.float32
        ).astype(jnp.bfloat16)
        each(group, c == 0, lambda device: give_back(device, me).start())
    returned[slots(me), :] = answer[slots(me), :]

    total = hid_ref[...].astype(jnp.float32)
    for c in range(groups):
        group = group_at(c)
        each(group, c == 0, lambda device: give_back(device, device).wait_recv())
        back = returned[group_rows(group), :]
        lanes = group_rows(group)
        total += jnp.dot(high_ref[:, lanes], back, preferred_element_type=jnp.float32)
        total += jnp.dot(low_ref[:, lanes], back, preferred_element_type=jnp.float32)
    new_ref[...] = total.astype(jnp.bfloat16)

    for c in range(groups):
        each(group_at(c), c == 0, lambda device: dispatch(device, me).wait_send())
        each(group_at(c), c == 0, lambda device: give_back(device, me).wait_send())


def run_experts(outgoing, high, low, hidden, gate_weight, up_weight, down_weight, capacity):
    n_tp = lax.axis_size("tp")
    devices = outgoing.shape[0] // capacity
    vmem = pl.BlockSpec(memory_space=pltpu.VMEM)
    anywhere = pl.BlockSpec(memory_space=pl.ANY)
    buffer = pltpu.VMEM(outgoing.shape, jnp.bfloat16)
    return pl.pallas_call(
        functools.partial(expert_kernel, n_tp, capacity),
        out_shape=jax.ShapeDtypeStruct(hidden.shape, jnp.bfloat16),
        in_specs=[vmem] * 4 + [anywhere] * 3,
        out_specs=vmem,
        scratch_shapes=[
            pltpu.VMEM(gate_weight.shape[1:], jnp.bfloat16),
            pltpu.VMEM(up_weight.shape[1:], jnp.bfloat16),
            pltpu.VMEM(down_weight.shape[1:], jnp.bfloat16),
            buffer,
            buffer,
            buffer,
            pltpu.SemaphoreType.DMA((devices,)),
            pltpu.SemaphoreType.DMA((devices,)),
            pltpu.SemaphoreType.DMA((devices,)),
            pltpu.SemaphoreType.DMA((devices,)),
            pltpu.SemaphoreType.DMA((3,)),
        ],
        compiler_params=pltpu.CompilerParams(
            collective_id=2, has_side_effects=True, vmem_limit_bytes=40 * 1024 * 1024
        ),
    )(outgoing, high, low, hidden, gate_weight, up_weight, down_weight)


def on_device(
    residual,
    query_proj,
    key_proj,
    value_proj,
    query_gain,
    key_gain,
    document_ids,
    output_weight,
    norm_gain,
    expert_ids,
    route_weights,
    gate_weight,
    up_weight,
    down_weight,
):
    rows_here = query_proj.shape[0]
    cosine, sine_table = rotary_tables(lax.axis_index("sp") * rows_here, rows_here)
    query_norm = norm_rotate(query_proj, query_gain, cosine, sine_table)
    key_norm = norm_rotate(key_proj, key_gain, cosine, sine_table)
    heads = query_proj.shape[1] // HEAD
    docs = document_ids.astype(jnp.float32)
    query_t = jnp.transpose(query_norm.reshape(rows_here, heads, HEAD), (1, 2, 0))
    query_doc = jnp.where(
        docs[None, :] == jnp.arange(HEAD, dtype=jnp.float32)[:, None], DOC_QUERY, 0.0
    ).astype(jnp.bfloat16)
    q_aug = jnp.concatenate(
        [query_t, jnp.broadcast_to(query_doc[None], (heads, HEAD, rows_here))], axis=1
    )
    doc_rows = jnp.broadcast_to(docs[None, :], (8, rows_here))
    hidden, normed = attend(
        q_aug, key_norm, value_proj.T, doc_rows, residual, norm_gain, output_weight
    )
    token_rows = residual.shape[0]
    top_count = expert_ids.shape[1]
    experts_all = lax.axis_size("sp") * lax.axis_size("tp")
    capacity = max(2, 2 * token_rows * top_count // experts_all)
    flat_ids = expert_ids.reshape(-1)
    order = jnp.arange(flat_ids.shape[0], dtype=jnp.int32)
    earlier = jnp.logical_and(
        flat_ids[:, None] == flat_ids[None, :], order[None, :] < order[:, None]
    )
    arrival = jnp.sum(earlier.astype(jnp.int32), axis=1)
    slot_index = flat_ids * capacity + arrival
    slot_grid = slot_index.reshape(token_rows, top_count)
    placing = jnp.sum(
        (
            jnp.arange(experts_all * capacity, dtype=jnp.int32)[:, None, None] == slot_grid[None]
        ).astype(jnp.float32),
        axis=2,
    ).astype(jnp.bfloat16)
    outgoing = jnp.dot(placing, normed, preferred_element_type=jnp.float32).astype(jnp.bfloat16)
    spread = jnp.sum(
        jnp.where(
            jnp.arange(experts_all * capacity, dtype=jnp.int32)[None, None, :]
            == slot_grid[:, :, None],
            route_weights[:, :, None],
            0.0,
        ),
        axis=1,
    )
    high = spread.astype(jnp.bfloat16)
    low = (spread - high.astype(jnp.float32)).astype(jnp.bfloat16)
    if capacity % 16 == 0 and token_rows % capacity == 0 and experts_all % (token_rows // capacity) == 0:
        return run_experts(
            outgoing, high, low, hidden, gate_weight, up_weight, down_weight, capacity
        )
    outgoing = outgoing.reshape(experts_all, capacity, normed.shape[1])
    arrived = lax.all_to_all(outgoing, ("sp", "tp"), split_axis=0, concat_axis=0, tiled=True)
    sources, slots, width = arrived.shape
    flat_rows = arrived.reshape(sources * slots, width)
    gate_part = jnp.dot(flat_rows, gate_weight[0], preferred_element_type=jnp.float32)
    up_part = jnp.dot(flat_rows, up_weight[0], preferred_element_type=jnp.float32)
    activity = (jax.nn.silu(gate_part) * up_part).astype(jnp.bfloat16)
    expert_out = jnp.dot(activity, down_weight[0], preferred_element_type=jnp.float32).astype(
        jnp.bfloat16
    )
    returned = lax.all_to_all(
        expert_out.reshape(sources, slots, width),
        ("sp", "tp"),
        split_axis=0,
        concat_axis=0,
        tiled=True,
    )
    rows_back = returned.reshape(experts_all * capacity, -1)
    combined = jnp.dot(high, rows_back, preferred_element_type=jnp.float32) + jnp.dot(
        low, rows_back, preferred_element_type=jnp.float32
    )
    return (hidden.astype(jnp.float32) + combined).astype(jnp.bfloat16)


def solution(mesh):
    in_specs = (
        P(("sp", "tp"), None),
        P("sp", "tp"),
        P("sp", "tp"),
        P("sp", "tp"),
        P(),
        P(),
        P("sp"),
        P(),
        P(),
        P(("sp", "tp"), None),
        P(("sp", "tp"), None),
        P(("sp", "tp"), None, None),
        P(("sp", "tp"), None, None),
        P(("sp", "tp"), None, None),
    )
    out_specs = P(("sp", "tp"), None)
    return jax.shard_map(
        on_device, mesh=mesh, in_specs=in_specs, out_specs=out_specs, check_vma=False
    )
```
